32 devices in a mesh: kv: 16 (over z, y, x), tp: 2 (over core).
Axes of the slice: x: 2, y: 2, z: 4, core: 2. Of those that a mesh axis runs over, the one named last changes fastest.
Arguments:
- tokens: bfloat16 [64, 2048], P('tp', 'kv'), may hold values from -60 to 60
- gain_mix: float32 [2048], P('kv'), may hold values from 0.1 to 1.9
- w_query: bfloat16 [2048, 2048], P('kv', 'tp'), may hold values from -0.125 to 0.125
- w_key: bfloat16 [2048, 2048], P('kv', 'tp'), may hold values from -0.125 to 0.125
- w_value: bfloat16 [2048, 2048], P('kv', 'tp'), may hold values from -0.125 to 0.125
- w_igate: bfloat16 [2048, 8], P('kv', 'tp'), may hold values from -0.125 to 0.125
- w_fgate: bfloat16 [2048, 8], P('kv', 'tp'), may hold values from -0.125 to 0.125
- bias_igate: float32 [8], P('tp'), may hold values from -3 to 3
- bias_fgate: float32 [8], P('tp'), may hold values from -3 to 3
- state_mem: float32 [64, 8, 256, 256], P('kv', 'tp'), may hold values from -2 to 2
- state_max: float32 [64, 8], P('kv', 'tp'), may hold values from -60 to 220
- keys_blk: bfloat16 [64, 8, 128, 256], P('kv', 'tp'), may hold values from -6 to 6
- values_blk: bfloat16 [64, 8, 128, 256], P('kv', 'tp'), may hold values from -6 to 6
- igate_blk: float32 [64, 8, 128], P('kv', 'tp'), may hold values from -10 to 220
- fgate_blk: float32 [64, 8, 128], P('kv', 'tp'), may hold values from -3 to 0
- lengths: int32 [64], P('kv'), may hold values from 1 to 127, 2048 in all
- gain_head: float32 [256], replicated, may hold values from 0.1 to 1.9
- w_mixout: bfloat16 [2048, 2048], P('tp', 'kv'), may hold values from -0.25 to 0.25
- gain_mlp: float32 [2048], P('kv'), may hold values from 0.1 to 1.9
- w_up: bfloat16 [2048, 8192], P('kv', 'tp'), may hold values from -0.125 to 0.125
- w_down: bfloat16 [8192, 2048], P('tp', 'kv'), may hold values from -0.0625 to 0.0625
Outputs:
- layer_out: bfloat16 [64, 2048], P('tp', 'kv')
The draws below stay inside these ranges and needn't reach their ends.
Inputs may be any that keep to these rules, and one draw needn't show every extreme that they name: `lengths`: entries of a sequence's block at or past its length are not live. The largest length is reached in every draw.
All inputs are finite; a program needn't handle non-finite values.
Results may differ from the reference program's by a relative error of at most 0.015.
Values may be sent and summed in bfloat16 or wider, within the bound.
No kernel may reach another device: no remote copies, remote signals or barrier semaphores. Data moves between devices by JAX's collectives and lax.ppermute only.
A program may use at most 64 MiB of HBM per device.

```python
import math
import jax
import jax.numpy as jnp
import numpy as np
from jax import lax

D = 2048
CELL_FACETS = 8
HD = 256
FF = 8192
SEGMENT_LENGTH = 128
STREAM_TOTAL = 64
D_ML = 2048
N_TP = 2


def draw_tokens(key, part):
    addressing_arrays = jax.random.split(key, 1)
    base = jax.random.normal(addressing_arrays[0], (STREAM_TOTAL, D), jnp.float32)
    columns = jnp.exp(jnp.log(0.4) + jnp.log(10.0) * jnp.arange(D, dtype=jnp.float32) / (D - 1))
    values = jnp.clip(base, -6.0, 6.0)
    return jnp.clip(values * columns[None, :], -60.0, 60.0).astype(jnp.bfloat16)


def draw_state_max(key, part):
    return jax.random.uniform(key, (STREAM_TOTAL, CELL_FACETS), jnp.float32, -1.0, 2.0)


def draw_igate_blk(key, part):
    addressing_arrays = jax.random.split(key, 1)
    return jnp.clip(jax.random.normal(addressing_arrays[0], (STREAM_TOTAL, CELL_FACETS, SEGMENT_LENGTH), jnp.float32), -6.0, 6.0)


def draw_fgate_blk(key, part):
    addressing_arrays = jax.random.split(key, 7)
    share = 0.5
    quick = jax.random.bernoulli(addressing_arrays[0], share, (STREAM_TOTAL, CELL_FACETS, 1))
    quick_rate = jax.random.uniform(addressing_arrays[1], (STREAM_TOTAL, CELL_FACETS, 1), jnp.float32, 2.0, 4.0) / 40.0
    slow_rate = jax.random.uniform(addressing_arrays[2], (STREAM_TOTAL, CELL_FACETS, 1), jnp.float32, 0.1, 0.8) / SEGMENT_LENGTH
    seqfactor = jnp.exp(jax.random.uniform(addressing_arrays[3], (STREAM_TOTAL, 1, 1), jnp.float32, jnp.log(0.5), jnp.log(2.0)))
    shrinking_quotient = jnp.where(quick, quick_rate, slow_rate) * seqfactor
    arbitrary_shift = jax.random.uniform(addressing_arrays[4], (STREAM_TOTAL, CELL_FACETS, SEGMENT_LENGTH), jnp.float32, 0.5, 1.5)
    segment_clusters = jax.random.bernoulli(addressing_arrays[5], 3.0 / SEGMENT_LENGTH, (STREAM_TOTAL, CELL_FACETS, SEGMENT_LENGTH))
    training_loss = jnp.log(jax.random.uniform(addressing_arrays[6], (STREAM_TOTAL, CELL_FACETS, SEGMENT_LENGTH), jnp.float32, 0.5, 0.8))
    return -shrinking_quotient * arbitrary_shift + jnp.where(segment_clusters, training_loss, 0.0)


def level_of(own_key, dims, cuts, least, high):
    gain, own = 1.0, jax.random.fold_in(own_key, 6)
    for position, blocks in cuts:
        draws = jnp.exp(jax.random.uniform(jax.random.fold_in(own, position), (blocks,), jnp.float32, least / len(cuts), high / len(cuts)))
        gain = gain * jnp.repeat(draws, dims[position] // blocks).reshape([-1 if axis == position else 1 for axis in range(len(dims))])
    return gain


def split_up(count, total, most, skew):
    portions = [(1 << 20) // math.isqrt(standing ** skew) + 1 for standing in range(2, count + 1)]
    rest, holding = total - most - (count - 1), [1] * (count - 1)
    while rest > 0:
        candidates = [i for i in range(count - 1) if holding[i] < most]
        whole, budget = sum([portions[i] for i in candidates]), rest
        for i in candidates:
            extra = min(most - holding[i], max(1, budget * portions[i] // whole), rest)
            holding[i] = holding[i] + extra
            rest = rest - extra
    return np.array([most] + holding)


def ragged(rng, amount, total, reach, lean):
    if amount == 2:
        one = jax.random.randint(rng, (), max(1, total - reach), min(reach, total - 1) + 1)
        return jnp.stack([one, total - one])
    sizes = jnp.asarray(split_up(amount, total, reach, lean), jnp.int32)
    couples = (amount - 1) // 2
    giver, sink = sizes[1:1 + 2 * couples:2], sizes[2:2 + 2 * couples:2]
    room = jnp.minimum(giver - 1, reach - sink)
    moved = jax.random.randint(jax.random.fold_in(rng, 1), (couples,), 0, 1 << 20) % (room + 1)
    sizes = sizes.at[1:1 + 2 * couples:2].set(giver - moved).at[2:2 + 2 * couples:2].set(sink + moved)
    return sizes[jax.random.permutation(jax.random.fold_in(rng, 2), amount)]


def noise(own_key, dims, width, limit, shards=(), kind=jnp.bfloat16):
    entries = jax.random.normal(own_key, dims, jnp.float32) * width
    if len(shards) > 0:
        entries = level_of(own_key, dims, shards, -0.22, 0.18) * entries
    return jnp.clip(entries, min=-limit, max=limit).astype(kind)


def setup_inputs(seed: int = 0) -> dict:
    key_of = jax.random.split(jax.random.key(seed), 22)
    return {
        "tokens": draw_tokens(jax.random.fold_in(key_of[21], 71), 0),
        "gain_mix": jnp.clip(1.0 + 0.18 * jax.random.normal(key_of[1], (D,), jnp.float32), 0.1, 1.9),
        "w_query": noise(key_of[2], (D, D_ML), D ** -0.5, 0.125, ((0, 16), (1, 2))),
        "w_key": noise(key_of[3], (D, D_ML), D ** -0.5, 0.125, ((0, 16), (1, 2))),
        "w_value": noise(key_of[4], (D, D_ML), D ** -0.5, 0.125, ((0, 16), (1, 2))),
        "w_igate": noise(key_of[5], (D, CELL_FACETS), D ** -0.5, 0.125, ((0, 16), (1, 2))),
        "w_fgate": noise(key_of[6], (D, CELL_FACETS), D ** -0.5, 0.125, ((0, 16), (1, 2))),
        "bias_igate": noise(key_of[7], (CELL_FACETS,), 1.0, 3.0, ((0, 2),), jnp.float32),
        "bias_fgate": noise(key_of[8], (CELL_FACETS,), 1.0, 3.0, ((0, 2),), jnp.float32),
        "state_mem": noise(key_of[9], (STREAM_TOTAL, CELL_FACETS, HD, HD), 0.3, 2.0, ((0, 16), (1, 2)), jnp.float32),
        "state_max": draw_state_max(jax.random.fold_in(key_of[21], 71), 0),
        "keys_blk": noise(key_of[11], (STREAM_TOTAL, CELL_FACETS, SEGMENT_LENGTH, HD), 1.0, 6.0, ((0, 16), (1, 2))),
        "values_blk": noise(key_of[12], (STREAM_TOTAL, CELL_FACETS, SEGMENT_LENGTH, HD), 1.0, 6.0, ((0, 16), (1, 2))),
        "igate_blk": draw_igate_blk(jax.random.fold_in(key_of[21], 71), 0),
        "fgate_blk": draw_fgate_blk(jax.random.fold_in(key_of[21], 71), 0),
        "lengths": ragged(key_of[15], STREAM_TOTAL, STREAM_TOTAL * SEGMENT_LENGTH // 4, SEGMENT_LENGTH - 1, 2).astype(jnp.int32),
        "gain_head": jnp.clip(1.0 + 0.18 * jax.random.normal(key_of[16], (HD,), jnp.float32), 0.1, 1.9),
        "w_mixout": noise(key_of[17], (D_ML, D), (D_ML // 4) ** -0.5, 0.25, ((0, 2), (1, 16))),
        "gain_mlp": jnp.clip(1.0 + 0.18 * jax.random.normal(key_of[18], (D,), jnp.float32), 0.1, 1.9),
        "w_up": noise(key_of[19], (D, FF), D ** -0.5, 0.125, ((0, 16), (1, 2))),
        "w_down": noise(key_of[20], (FF, D), FF ** -0.5, 0.0625, ((0, 2), (1, 16))),
    }


EPS = 1e-06

def rms_factor(values):
    return lax.rsqrt(lax.optimization_barrier(jnp.mean(values * values, axis=-1, keepdims=True)) + EPS)

def memory_cell(query, key_new, value_new, input_gate, forget_gate, state_mem, state_max, keys_blk, values_blk, igate_blk, fgate_blk, lengths, gain_head):
    span = keys_blk.shape[2]
    head_size = query.shape[-1]
    positions = jnp.arange(span, dtype=jnp.int32)
    live_mask = positions[None, None, :] < lengths.astype(jnp.int32)[:, None, None]
    forget_live = jnp.where(live_mask, fgate_blk, 0.0)
    cumulative = jnp.cumsum(forget_live, axis=-1)
    total = cumulative[..., -1]
    suffix = total[..., None] - cumulative + forget_gate[..., None]
    past = igate_blk + suffix
    carried = state_max + total + forget_gate
    topmost = jnp.maximum(jnp.maximum(carried, input_gate), lax.optimization_barrier(jnp.max(jnp.where(live_mask, past, -jnp.inf), axis=-1)))
    scale = head_size ** (-0.5)
    query_f = query.astype(jnp.float32)
    scores = jnp.einsum('bhd,bhsd->bhs', query_f, keys_blk.astype(jnp.float32)) * scale
    weights = (jnp.where(live_mask, jnp.exp(past - topmost[..., None]), 0.0) * scores).astype(jnp.bfloat16)
    block_term = jnp.einsum('bhs,bhsd->bhd', weights.astype(jnp.float32), values_blk.astype(jnp.float32))
    state_term = jnp.einsum('bhvk,bhk->bhv', state_mem, query_f, precision=lax.Precision.HIGHEST) * jnp.exp(carried - topmost)[..., None]
    own_score = lax.optimization_barrier(jnp.sum(query_f * key_new.astype(jnp.float32), axis=-1)) * scale
    own_term = (jnp.exp(input_gate - topmost) * own_score)[..., None] * value_new.astype(jnp.float32)
    numerator = state_term + block_term + own_term
    normed = numerator * rms_factor(numerator) * gain_head
    return normed.astype(jnp.bfloat16).reshape(query.shape[0], -1)

def grouped_sum(left, right):
    left_groups = left.reshape(left.shape[0], N_TP, -1).astype(jnp.float32)
    right_groups = right.reshape(N_TP, -1, right.shape[1]).astype(jnp.float32)
    partials = jnp.einsum('bgc,gcd->gbd', left_groups, right_groups)
    rounded = lax.optimization_barrier(partials.astype(jnp.bfloat16))
    return lax.optimization_barrier(jnp.sum(rounded.astype(jnp.float32), axis=0))

def reference(tokens, gain_mix, w_query, w_key, w_value, w_igate, w_fgate, bias_igate, bias_fgate, state_mem, state_max, keys_blk, values_blk, igate_blk, fgate_blk, lengths, gain_head, w_mixout, gain_mlp, w_up, w_down):
    widened = tokens.astype(jnp.float32)
    factor_in = rms_factor(widened)
    scaled_in = (widened * gain_mix).astype(jnp.bfloat16)

    def project(weight):
        return jnp.dot(scaled_in, weight, preferred_element_type=jnp.float32) * factor_in
    query = project(w_query).astype(jnp.bfloat16).reshape(STREAM_TOTAL, CELL_FACETS, HD)
    key_new = project(w_key).astype(jnp.bfloat16).reshape(STREAM_TOTAL, CELL_FACETS, HD)
    value_new = project(w_value).astype(jnp.bfloat16).reshape(STREAM_TOTAL, CELL_FACETS, HD)
    input_gate = project(w_igate) + bias_igate
    forget_gate = jax.nn.log_sigmoid(project(w_fgate) + bias_fgate)
    mixed = memory_cell(query, key_new, value_new, input_gate, forget_gate, state_mem, state_max, keys_blk, values_blk, igate_blk, fgate_blk, lengths, gain_head)
    attended = grouped_sum(mixed, w_mixout)
    residual = (widened + attended).astype(jnp.bfloat16)
    restored = residual.astype(jnp.float32)
    factor_mid = rms_factor(restored)
    scaled_mid = (restored * gain_mlp).astype(jnp.bfloat16)
    upward = jnp.dot(scaled_mid, w_up, preferred_element_type=jnp.float32) * factor_mid
    hidden = jnp.square(jax.nn.relu(upward)).astype(jnp.bfloat16)
    return (restored + grouped_sum(hidden, w_down)).astype(jnp.bfloat16)
```

```python
import jax
import jax.numpy as jnp
from jax import lax
from jax.sharding import PartitionSpec as P

D = 2048


EPS = 1e-06
LANES = 128


def memory_cell(
    query,
    key_new,
    value_new,
    input_gate,
    forget_gate,
    state_mem,
    state_max,
    keys_blk,
    values_blk,
    igate_blk,
    fgate_blk,
    lengths,
    gain_head,
):
    span = keys_blk.shape[2]
    head_size = query.shape[-1]
    positions = jnp.arange(span, dtype=jnp.int32)
    live_mask = positions[None, None, :] < lengths[:, None, None]
    forget_live = jnp.where(live_mask, fgate_blk, 0.0)
    cumulative = jnp.cumsum(forget_live, axis=-1)
    total = cumulative[..., -1]
    suffix = total[..., None] - cumulative + forget_gate[..., None]
    past = igate_blk + suffix
    carried = state_max + total + forget_gate
    topmost = jnp.maximum(
        jnp.maximum(carried, input_gate), jnp.max(jnp.where(live_mask, past, -jnp.inf), axis=-1)
    )
    scale = head_size ** (-0.5)
    scores = (
        jnp.einsum("shd,shbd->shb", query, keys_blk, preferred_element_type=jnp.float32) * scale
    )
    weights = (jnp.where(live_mask, jnp.exp(past - topmost[..., None]), 0.0) * scores).astype(
        jnp.bfloat16
    )
    block_term = jnp.einsum(
        "shb,shbd->shd", weights, values_blk, preferred_element_type=jnp.float32
    )
    query_f = query.astype(jnp.float32)
    state_term = (
        jnp.einsum("shvk,shk->shv", state_mem, query_f, precision=lax.Precision.HIGHEST)
        * jnp.exp(carried - topmost)[..., None]
    )
    own_score = jnp.sum(query_f * key_new.astype(jnp.float32), axis=-1) * scale
    own_term = (jnp.exp(input_gate - topmost) * own_score)[..., None] * value_new.astype(
        jnp.float32
    )
    numerator = state_term + block_term + own_term
    normed = (
        numerator
        * lax.rsqrt(jnp.mean(numerator * numerator, axis=-1, keepdims=True) + EPS)
        * gain_head
    )
    return normed.astype(jnp.bfloat16).reshape(query.shape[0], -1)


def pieces(values):
    first = lax.reduce_precision(values, 8, 7)
    rest = values - first
    second = lax.reduce_precision(rest, 8, 7)
    third = lax.reduce_precision(rest - second, 8, 7)
    return jnp.concatenate([first, second, third], axis=1).astype(jnp.bfloat16)


def with_extras(main, extras):
    packed = pieces(extras)
    pad = -packed.shape[1] % LANES
    return jnp.concatenate(
        [main.astype(jnp.bfloat16), jnp.pad(packed, ((0, 0), (0, pad)))], axis=1
    )


def scatter_sum(packed, width, extra_count):
    peers = lax.axis_size("kv")
    blocks = packed.reshape(peers, packed.shape[0] // peers, packed.shape[1])
    received = lax.all_to_all(blocks, "kv", 0, 0, tiled=True)
    total = jnp.sum(received.astype(jnp.float32), axis=0)
    extras = total[:, width : width + 3 * extra_count]
    extras = extras.reshape(total.shape[0], 3, extra_count)
    return total[:, :width], extras[:, 0] + (extras[:, 1] + extras[:, 2])


def gather_rows(rows):
    peers = lax.axis_size("kv")
    copies = jnp.broadcast_to(rows[None], (peers,) + rows.shape)
    return lax.all_to_all(copies, "kv", 0, 0, tiled=True).reshape(-1, rows.shape[1])


def tp_sum(partial):
    if lax.axis_size("tp") != 2:
        return lax.psum(partial, "tp").astype(jnp.float32)
    other = lax.ppermute(partial, "tp", [(0, 1), (1, 0)])
    return partial.astype(jnp.float32) + other.astype(jnp.float32)


def tp_scatter_sum(partial, row_count):
    if lax.axis_size("tp") != 2:
        return lax.psum_scatter(partial, "tp", scatter_dimension=0, tiled=True).astype(
            jnp.float32
        )
    side = lax.axis_index("tp")
    own = lax.dynamic_slice_in_dim(partial, side * row_count, row_count, 0)
    away = lax.dynamic_slice_in_dim(partial, (1 - side) * row_count, row_count, 0)
    other = lax.ppermute(away, "tp", [(0, 1), (1, 0)])
    return own.astype(jnp.float32) + other.astype(jnp.float32)


def body(
    tokens,
    gain_mix,
    w_query,
    w_key,
    w_value,
    w_igate,
    w_fgate,
    bias_igate,
    bias_fgate,
    state_mem,
    state_max,
    keys_blk,
    values_blk,
    igate_blk,
    fgate_blk,
    lengths,
    gain_head,
    w_mixout,
    gain_mlp,
    w_up,
    w_down,
):
    sequences = state_mem.shape[0]
    head_count = state_mem.shape[1]
    head_size = state_mem.shape[3]
    inner_width = head_count * head_size
    gathered = lax.all_gather(tokens, "tp", axis=0, tiled=True)
    widened = gathered.astype(jnp.float32)
    square_in = jnp.sum(widened * widened, axis=1)
    scaled_in = (widened * gain_mix).astype(jnp.bfloat16)
    w_main = jnp.concatenate([w_query, w_key, w_value], axis=1)
    w_gates = jnp.concatenate([w_igate, w_fgate], axis=1)
    main_part = jnp.dot(scaled_in, w_main, preferred_element_type=jnp.float32)
    gate_part = jnp.dot(scaled_in, w_gates, preferred_element_type=jnp.float32)
    extras_in = jnp.concatenate([gate_part, square_in[:, None]], axis=1)
    main_sum, extra_sum = scatter_sum(
        with_extras(main_part, extras_in), main_part.shape[1], extras_in.shape[1]
    )
    gate_sum = extra_sum[:, : 2 * head_count]
    square_mine = extra_sum[:, 2 * head_count]
    factor_in = lax.rsqrt(square_mine / D + EPS)[:, None]
    projected = main_sum * factor_in
    query = (
        projected[:, :inner_width].astype(jnp.bfloat16).reshape(sequences, head_count, head_size)
    )
    key_new = (
        projected[:, inner_width : 2 * inner_width]
        .astype(jnp.bfloat16)
        .reshape(sequences, head_count, head_size)
    )
    value_new = (
        projected[:, 2 * inner_width :]
        .astype(jnp.bfloat16)
        .reshape(sequences, head_count, head_size)
    )
    gate_scaled = gate_sum * factor_in
    input_gate = gate_scaled[:, :head_count] + bias_igate
    forget_gate = jax.nn.log_sigmoid(gate_scaled[:, head_count:] + bias_fgate)
    mixed = memory_cell(
        query,
        key_new,
        value_new,
        input_gate,
        forget_gate,
        state_mem,
        state_max,
        keys_blk,
        values_blk,
        igate_blk,
        fgate_blk,
        lengths,
        gain_head,
    )
    partial_value = jnp.dot(
        gather_rows(mixed),
        w_mixout,
        preferred_element_type=jnp.float32,
    )
    attended = tp_sum(partial_value.astype(jnp.bfloat16))
    residual = (widened + attended).astype(jnp.bfloat16)
    restored = residual.astype(jnp.float32)
    square_mid = jnp.sum(restored * restored, axis=1, keepdims=True)
    scaled_mid = (restored * gain_mlp).astype(jnp.bfloat16)
    up_part = jnp.dot(scaled_mid, w_up, preferred_element_type=jnp.float32)
    up_sum, square_sum = scatter_sum(with_extras(up_part, square_mid), up_part.shape[1], 1)
    hidden = jnp.square(jax.nn.relu(up_sum * lax.rsqrt(square_sum / D + EPS))).astype(
        jnp.bfloat16
    )
    down_part = jnp.dot(gather_rows(hidden), w_down, preferred_element_type=jnp.float32)
    row_count = tokens.shape[0]
    down_sum = tp_scatter_sum(down_part.astype(jnp.bfloat16), row_count)
    own_rows = lax.dynamic_slice_in_dim(restored, lax.axis_index("tp") * row_count, row_count, 0)
    return (own_rows + down_sum).astype(jnp.bfloat16)


def solution(mesh):
    in_specs = (
        P("tp", "kv"),
        P("kv"),
        P("kv", "tp"),
        P("kv", "tp"),
        P("kv", "tp"),
        P("kv", "tp"),
        P("kv", "tp"),
        P("tp"),
        P("tp"),
        P("kv", "tp", None, None),
        P("kv", "tp"),
        P("kv", "tp", None, None),
        P("kv", "tp", None, None),
        P("kv", "tp", None),
        P("kv", "tp", None),
        P("kv"),
        P(),
        P("tp", "kv"),
        P("kv"),
        P("kv", "tp"),
        P("tp", "kv"),
    )
    out_specs = P("tp", "kv")
    return jax.shard_map(body, mesh=mesh, in_specs=in_specs, out_specs=out_specs, check_vma=False)
```

```python
import jax
import jax.numpy as jnp
from jax import lax
from jax.sharding import PartitionSpec as P

D = 2048


EPS = 1e-06
LANES = 128


def memory_cell(
    query,
    key_new,
    value_new,
    input_gate,
    forget_gate,
    state_mem,
    state_max,
    keys_blk,
    values_blk,
    igate_blk,
    live_mask,
    later,
    total,
    gain_head,
):
    head_size = query.shape[-1]
    suffix = later + forget_gate[..., None]
    past = igate_blk + suffix
    carried = state_max + total + forget_gate
    topmost = jnp.maximum(
        jnp.maximum(carried, input_gate), jnp.max(jnp.where(live_mask, past, -jnp.inf), axis=-1)
    )
    scale = head_size ** (-0.5)
    scores = (
        jnp.einsum("shd,shbd->shb", query, keys_blk, preferred_element_type=jnp.float32) * scale
    )
    weights = (jnp.where(live_mask, jnp.exp(past - topmost[..., None]), 0.0) * scores).astype(
        jnp.bfloat16
    )
    block_term = jnp.einsum(
        "shb,shbd->shd", weights, values_blk, preferred_element_type=jnp.float32
    )
    query_f = query.astype(jnp.float32)
    state_term = (
        jnp.einsum(
            "shvk,shk->shv",
            state_mem.astype(jnp.bfloat16),
            query,
            preferred_element_type=jnp.float32,
        )
        * jnp.exp(carried - topmost)[..., None]
    )
    own_score = jnp.sum(query_f * key_new.astype(jnp.float32), axis=-1) * scale
    own_term = (jnp.exp(input_gate - topmost) * own_score)[..., None] * value_new.astype(
        jnp.float32
    )
    numerator = state_term + block_term + own_term
    normed = (
        numerator
        * lax.rsqrt(jnp.mean(numerator * numerator, axis=-1, keepdims=True) + EPS)
        * gain_head
    )
    return normed.astype(jnp.bfloat16).reshape(query.shape[0], -1)


def pieces(values):
    first = lax.reduce_precision(values, 8, 7)
    rest = values - first
    second = lax.reduce_precision(rest, 8, 7)
    third = lax.reduce_precision(rest - second, 8, 7)
    return jnp.concatenate([first, second, third], axis=1).astype(jnp.bfloat16)


def with_extras(main, extras):
    packed = pieces(extras)
    pad = -packed.shape[1] % LANES
    return jnp.concatenate(
        [main.astype(jnp.bfloat16), jnp.pad(packed, ((0, 0), (0, pad)))], axis=1
    )


def scatter_sum(packed, width, extra_count):
    peers = lax.axis_size("kv")
    blocks = packed.reshape(peers, packed.shape[0] // peers, packed.shape[1])
    received = lax.all_to_all(blocks, "kv", 0, 0, tiled=True)
    total = jnp.sum(received.astype(jnp.float32), axis=0)
    extras = total[:, width : width + 3 * extra_count]
    extras = extras.reshape(total.shape[0], 3, extra_count)
    return total[:, :width], extras[:, 0] + (extras[:, 1] + extras[:, 2])


def gather_rows(rows):
    peers = lax.axis_size("kv")
    copies = jnp.broadcast_to(rows[None], (peers,) + rows.shape)
    return lax.all_to_all(copies, "kv", 0, 0, tiled=True).reshape(-1, rows.shape[1])


def tp_sum(partial):
    if lax.axis_size("tp") != 2:
        return lax.psum(partial, "tp").astype(jnp.float32)
    other = lax.ppermute(partial, "tp", [(0, 1), (1, 0)])
    return partial.astype(jnp.float32) + other.astype(jnp.float32)


def half_of(rows, row_count, lower):
    return jnp.where(lower, rows[:row_count], rows[row_count:])


def own_half(rows, row_count, first_side):
    if lax.axis_size("tp") != 2:
        return lax.dynamic_slice_in_dim(rows, lax.axis_index("tp") * row_count, row_count, 0)
    return half_of(rows, row_count, first_side)


def tp_scatter_sum(partial, row_count, first_side):
    if lax.axis_size("tp") != 2:
        return lax.psum_scatter(partial, "tp", scatter_dimension=0, tiled=True).astype(
            jnp.float32
        )
    own = half_of(partial, row_count, first_side)
    away = jnp.where(first_side, partial[row_count:], partial[:row_count])
    other = lax.ppermute(away, "tp", [(0, 1), (1, 0)])
    return own.astype(jnp.float32) + other.astype(jnp.float32)


def block_gates(fgate_blk, lengths):
    span = fgate_blk.shape[2]
    positions = jnp.arange(span, dtype=jnp.int32)
    live_mask = positions[None, None, :] < lengths[:, None, None]
    forget_live = jnp.where(live_mask, fgate_blk, 0.0)
    after = (positions[:, None] > positions[None, :]).astype(jnp.float32)
    later = jnp.einsum("shj,jp->shp", forget_live, after, precision=lax.Precision.HIGHEST)
    return live_mask, later, jnp.sum(forget_live, axis=-1)


def body(
    tokens,
    gain_mix,
    w_query,
    w_key,
    w_value,
    w_igate,
    w_fgate,
    bias_igate,
    bias_fgate,
    state_mem,
    state_max,
    keys_blk,
    values_blk,
    igate_blk,
    fgate_blk,
    lengths,
    gain_head,
    w_mixout,
    gain_mlp,
    w_up,
    w_down,
):
    sequences = state_mem.shape[0]
    head_count = state_mem.shape[1]
    head_size = state_mem.shape[3]
    inner_width = head_count * head_size
    first_side = lax.axis_index("tp") == 0
    live_mask, later, total = block_gates(fgate_blk, lengths)
    gathered = lax.all_gather(tokens, "tp", axis=0, tiled=True)
    widened = gathered.astype(jnp.float32)
    square_in = jnp.sum(widened * widened, axis=1)
    scaled_in = (widened * gain_mix).astype(jnp.bfloat16)
    w_main = jnp.concatenate([w_query, w_key, w_value], axis=1)
    w_gates = jnp.concatenate([w_igate, w_fgate], axis=1)
    main_part = jnp.dot(scaled_in, w_main, preferred_element_type=jnp.float32)
    gate_part = jnp.dot(scaled_in, w_gates, preferred_element_type=jnp.float32)
    extras_in = jnp.concatenate([gate_part, square_in[:, None]], axis=1)
    packed, first_side, live_mask, later, total = lax.optimization_barrier(
        (with_extras(main_part, extras_in), first_side, live_mask, later, total)
    )
    main_sum, extra_sum = scatter_sum(packed, main_part.shape[1], extras_in.shape[1])
    gate_sum = extra_sum[:, : 2 * head_count]
    square_mine = extra_sum[:, 2 * head_count]
    factor_in = lax.rsqrt(square_mine / D + EPS)[:, None]
    projected = main_sum * factor_in
    query = (
        projected[:, :inner_width].astype(jnp.bfloat16).reshape(sequences, head_count, head_size)
    )
    key_new = (
        projected[:, inner_width : 2 * inner_width]
        .astype(jnp.bfloat16)
        .reshape(sequences, head_count, head_size)
    )
    value_new = (
        projected[:, 2 * inner_width :]
        .astype(jnp.bfloat16)
        .reshape(sequences, head_count, head_size)
    )
    gate_scaled = gate_sum * factor_in
    input_gate = gate_scaled[:, :head_count] + bias_igate
    forget_gate = jax.nn.log_sigmoid(gate_scaled[:, head_count:] + bias_fgate)
    mixed = memory_cell(
        query,
        key_new,
        value_new,
        input_gate,
        forget_gate,
        state_mem,
        state_max,
        keys_blk,
        values_blk,
        igate_blk,
        live_mask,
        later,
        total,
        gain_head,
    )
    partial_value = jnp.dot(
        gather_rows(mixed),
        w_mixout,
        preferred_element_type=jnp.float32,
    )
    attended = tp_sum(partial_value.astype(jnp.bfloat16))
    residual = (widened + attended).astype(jnp.bfloat16)
    restored = residual.astype(jnp.float32)
    square_mid = jnp.sum(restored * restored, axis=1, keepdims=True)
    scaled_mid = (restored * gain_mlp).astype(jnp.bfloat16)
    up_part = jnp.dot(scaled_mid, w_up, preferred_element_type=jnp.float32)
    up_sum, square_sum = scatter_sum(with_extras(up_part, square_mid), up_part.shape[1], 1)
    hidden = jnp.square(jax.nn.relu(up_sum * lax.rsqrt(square_sum / D + EPS))).astype(
        jnp.bfloat16
    )
    down_part = jnp.dot(gather_rows(hidden), w_down, preferred_element_type=jnp.float32)
    row_count = tokens.shape[0]
    down_sum = tp_scatter_sum(down_part.astype(jnp.bfloat16), row_count, first_side)
    own_rows = own_half(restored, row_count, first_side)
    return (own_rows + down_sum).astype(jnp.bfloat16)


def solution(mesh):
    in_specs = (
        P("tp", "kv"),
        P("kv"),
        P("kv", "tp"),
        P("kv", "tp"),
        P("kv", "tp"),
        P("kv", "tp"),
        P("kv", "tp"),
        P("tp"),
        P("tp"),
        P("kv", "tp", None, None),
        P("kv", "tp"),
        P("kv", "tp", None, None),
        P("kv", "tp", None, None),
        P("kv", "tp", None),
        P("kv", "tp", None),
        P("kv"),
        P(),
        P("tp", "kv"),
        P("kv"),
        P("kv", "tp"),
        P("tp", "kv"),
    )
    out_specs = P("tp", "kv")
    return jax.shard_map(body, mesh=mesh, in_specs=in_specs, out_specs=out_specs, check_vma=False)
```

```python
import jax
import jax.numpy as jnp
from jax import lax
from jax.sharding import PartitionSpec as P

D = 2048


EPS = 1e-06
LANES = 128


def memory_cell(
    query,
    key_new,
    value_new,
    input_gate,
    forget_gate,
    state_mem,
    state_max,
    keys_blk,
    values_blk,
    igate_blk,
    live_mask,
    later,
    total,
    gain_head,
):
    head_size = query.shape[-1]
    suffix = later + forget_gate[..., None]
    past = igate_blk + suffix
    carried = state_max + total + forget_gate
    topmost = jnp.maximum(
        jnp.maximum(carried, input_gate), jnp.max(jnp.where(live_mask, past, -jnp.inf), axis=-1)
    )
    scale = head_size ** (-0.5)
    scores = (
        jnp.einsum("shd,shbd->shb", query, keys_blk, preferred_element_type=jnp.float32) * scale
    )
    weights = (jnp.where(live_mask, jnp.exp(past - topmost[..., None]), 0.0) * scores).astype(
        jnp.bfloat16
    )
    block_term = jnp.einsum(
        "shb,shbd->shd", weights, values_blk, preferred_element_type=jnp.float32
    )
    query_f = query.astype(jnp.float32)
    state_term = (
        jnp.einsum(
            "shvk,shk->shv",
            state_mem.astype(jnp.bfloat16),
            query,
            preferred_element_type=jnp.float32,
        )
        * jnp.exp(carried - topmost)[..., None]
    )
    own_score = jnp.sum(query_f * key_new.astype(jnp.float32), axis=-1) * scale
    own_term = (jnp.exp(input_gate - topmost) * own_score)[..., None] * value_new.astype(
        jnp.float32
    )
    numerator = state_term + block_term + own_term
    normed = (
        numerator
        * lax.rsqrt(jnp.mean(numerator * numerator, axis=-1, keepdims=True) + EPS)
        * gain_head
    )
    return normed.astype(jnp.bfloat16).reshape(query.shape[0], -1)


def pieces(values):
    first = lax.reduce_precision(values, 8, 7)
    rest = values - first
    second = lax.reduce_precision(rest, 8, 7)
    third = lax.reduce_precision(rest - second, 8, 7)
    return jnp.concatenate([first, second, third], axis=1).astype(jnp.bfloat16)


def with_extras(main, extras):
    packed = pieces(extras)
    pad = -packed.shape[1] % LANES
    return jnp.concatenate(
        [main.astype(jnp.bfloat16), jnp.pad(packed, ((0, 0), (0, pad)))], axis=1
    )


def scatter_sum(packed, width, extra_count):
    peers = lax.axis_size("kv")
    blocks = packed.reshape(peers, packed.shape[0] // peers, packed.shape[1])
    received = lax.all_to_all(blocks, "kv", 0, 0, tiled=True)
    total = jnp.sum(received.astype(jnp.float32), axis=0)
    extras = total[:, width : width + 3 * extra_count]
    extras = extras.reshape(total.shape[0], 3, extra_count)
    return total[:, :width], extras[:, 0] + (extras[:, 1] + extras[:, 2])


def gather_rows(rows):
    peers = lax.axis_size("kv")
    copies = jnp.broadcast_to(rows[None], (peers,) + rows.shape)
    return lax.all_to_all(copies, "kv", 0, 0, tiled=True).reshape(-1, rows.shape[1])


def tp_sum(partial):
    if lax.axis_size("tp") != 2:
        return lax.psum(partial, "tp").astype(jnp.float32)
    other = lax.ppermute(partial, "tp", [(0, 1), (1, 0)])
    return partial.astype(jnp.float32) + other.astype(jnp.float32)


def half_of(rows, row_count, lower):
    return jnp.where(lower, rows[:row_count], rows[row_count:])


def own_half(rows, row_count, first_side):
    if lax.axis_size("tp") != 2:
        return lax.dynamic_slice_in_dim(rows, lax.axis_index("tp") * row_count, row_count, 0)
    return half_of(rows, row_count, first_side)


def tp_scatter_sum(partial, row_count, first_side):
    if lax.axis_size("tp") != 2:
        return lax.psum_scatter(partial, "tp", scatter_dimension=0, tiled=True).astype(
            jnp.float32
        )
    own = half_of(partial, row_count, first_side)
    away = jnp.where(first_side, partial[row_count:], partial[:row_count])
    other = lax.ppermute(away, "tp", [(0, 1), (1, 0)])
    return own.astype(jnp.float32) + other.astype(jnp.float32)


def block_gates(fgate_blk, lengths):
    span = fgate_blk.shape[2]
    positions = jnp.arange(span, dtype=jnp.int32)
    live_mask = positions[None, None, :] < lengths[:, None, None]
    forget_live = jnp.where(live_mask, fgate_blk, 0.0)
    after = (positions[:, None] > positions[None, :]).astype(jnp.float32)
    later = jnp.einsum("shj,jp->shp", forget_live, after, precision=lax.Precision.HIGHEST)
    return live_mask, later, jnp.sum(forget_live, axis=-1)


def body(
    tokens,
    gain_mix,
    w_query,
    w_key,
    w_value,
    w_igate,
    w_fgate,
    bias_igate,
    bias_fgate,
    state_mem,
    state_max,
    keys_blk,
    values_blk,
    igate_blk,
    fgate_blk,
    lengths,
    gain_head,
    w_mixout,
    gain_mlp,
    w_up,
    w_down,
):
    sequences = state_mem.shape[0]
    head_count = state_mem.shape[1]
    head_size = state_mem.shape[3]
    inner_width = head_count * head_size
    first_side = lax.axis_index("tp") == 0
    gathered = lax.all_gather(tokens, "tp", axis=0, tiled=True)
    widened = gathered.astype(jnp.float32)
    square_in = jnp.sum(widened * widened, axis=1)
    scaled_in = (widened * gain_mix).astype(jnp.bfloat16)
    w_main = jnp.concatenate([w_query, w_key, w_value], axis=1)
    main_part = jnp.dot(scaled_in, w_main, preferred_element_type=jnp.float32)
    main_part, w_igate, w_fgate = lax.optimization_barrier(
        (main_part.astype(jnp.bfloat16), w_igate, w_fgate)
    )
    w_gates = jnp.concatenate([w_igate, w_fgate], axis=1)
    gate_part = jnp.dot(scaled_in, w_gates, preferred_element_type=jnp.float32)
    extras_in = jnp.concatenate([gate_part, square_in[:, None]], axis=1)
    packed, first_side = lax.optimization_barrier(
        (with_extras(main_part, extras_in), first_side)
    )
    main_sum, extra_sum = scatter_sum(packed, main_part.shape[1], extras_in.shape[1])
    main_sum, extra_sum, fgate_blk, lengths = lax.optimization_barrier(
        (main_sum, extra_sum, fgate_blk, lengths)
    )
    live_mask, later, total = block_gates(fgate_blk, lengths)
    gate_sum = extra_sum[:, : 2 * head_count]
    square_mine = extra_sum[:, 2 * head_count]
    factor_in = lax.rsqrt(square_mine / D + EPS)[:, None]
    projected = main_sum * factor_in
    query = (
        projected[:, :inner_width].astype(jnp.bfloat16).reshape(sequences, head_count, head_size)
    )
    key_new = (
        projected[:, inner_width : 2 * inner_width]
        .astype(jnp.bfloat16)
        .reshape(sequences, head_count, head_size)
    )
    value_new = (
        projected[:, 2 * inner_width :]
        .astype(jnp.bfloat16)
        .reshape(sequences, head_count, head_size)
    )
    gate_scaled = gate_sum * factor_in
    input_gate = gate_scaled[:, :head_count] + bias_igate
    forget_gate = jax.nn.log_sigmoid(gate_scaled[:, head_count:] + bias_fgate)
    mixed = memory_cell(
        query,
        key_new,
        value_new,
        input_gate,
        forget_gate,
        state_mem,
        state_max,
        keys_blk,
        values_blk,
        igate_blk,
        live_mask,
        later,
        total,
        gain_head,
    )
    partial_value = jnp.dot(
        gather_rows(mixed),
        w_mixout,
        preferred_element_type=jnp.float32,
    )
    attended = tp_sum(partial_value.astype(jnp.bfloat16))
    residual = (widened + attended).astype(jnp.bfloat16)
    restored = residual.astype(jnp.float32)
    square_mid = jnp.sum(restored * restored, axis=1, keepdims=True)
    scaled_mid = (restored * gain_mlp).astype(jnp.bfloat16)
    up_part = jnp.dot(scaled_mid, w_up, preferred_element_type=jnp.float32)
    up_sum, square_sum = scatter_sum(with_extras(up_part, square_mid), up_part.shape[1], 1)
    hidden = jnp.square(jax.nn.relu(up_sum * lax.rsqrt(square_sum / D + EPS))).astype(
        jnp.bfloat16
    )
    down_part = jnp.dot(gather_rows(hidden), w_down, preferred_element_type=jnp.float32)
    row_count = tokens.shape[0]
    down_sum = tp_scatter_sum(down_part.astype(jnp.bfloat16), row_count, first_side)
    own_rows = own_half(restored, row_count, first_side)
    return (own_rows + down_sum).astype(jnp.bfloat16)


def solution(mesh):
    in_specs = (
        P("tp", "kv"),
        P("kv"),
        P("kv", "tp"),
        P("kv", "tp"),
        P("kv", "tp"),
        P("kv", "tp"),
        P("kv", "tp"),
        P("tp"),
        P("tp"),
        P("kv", "tp", None, None),
        P("kv", "tp"),
        P("kv", "tp", None, None),
        P("kv", "tp", None, None),
        P("kv", "tp", None),
        P("kv", "tp", None),
        P("kv"),
        P(),
        P("tp", "kv"),
        P("kv"),
        P("kv", "tp"),
        P("tp", "kv"),
    )
    out_specs = P("tp", "kv")
    return jax.shard_map(body, mesh=mesh, in_specs=in_specs, out_specs=out_specs, check_vma=False)
```
